32 devices in a mesh: ep: 8 (over z, y), tp: 4 (over x, core).
Axes of the slice: x: 2, y: 2, z: 4, core: 2. Of those that a mesh axis runs over, the one named last changes fastest.
Arguments:
- tokens: bfloat16 [192, 2048], P('ep'), may hold values from -6 to 6
- norm_attn: float32 [2048], replicated, may hold values from 0.1 to 1.9
- w_query: bfloat16 [2048, 2048], P(None, 'tp'), may hold values from -0.125 to 0.125
- w_key: bfloat16 [2048, 256], P(None, 'tp'), may hold values from -0.125 to 0.125
- w_value: bfloat16 [2048, 256], P(None, 'tp'), may hold values from -0.125 to 0.125
- w_out: bfloat16 [2048, 2048], P('tp'), may hold values from -1 to 1
- head_bias: float32 [32], P('tp'), may hold values from -7 to -3
- key_cache: bfloat16 [192, 4, 1024, 64], P('ep', 'tp'), may hold values from -6 to 6
- value_cache: bfloat16 [192, 4, 1024, 64], P('ep', 'tp'), may hold values from -6 to 6
- lengths: int32 [192], P('ep'), may hold values from 1 to 1024, 98304 in all
- norm_ffn: float32 [2048], replicated, may hold values from 0.1 to 1.9
- w_group: bfloat16 [2048, 4], replicated, may hold values from -0.125 to 0.125
- w_fine: bfloat16 [2048, 8], replicated, may hold values from -0.125 to 0.125
- routes: int32 [192, 2], P('ep'), may hold values from 0 to 7, as said below
- e_gate: bfloat16 [8, 2048, 512], P('ep', 'tp'), may hold values from -0.125 to 0.125
- e_up: bfloat16 [8, 2048, 512], P('ep', 'tp'), may hold values from -0.125 to 0.125
- e_down: bfloat16 [8, 512, 2048], P('ep', None, 'tp'), may hold values from -1 to 1
- d_gate: bfloat16 [2048, 8192], P('tp', 'ep'), may hold values from -0.125 to 0.125
- d_up: bfloat16 [2048, 8192], P('tp', 'ep'), may hold values from -0.125 to 0.125
- d_down: bfloat16 [8192, 2048], P('ep', 'tp'), may hold values from -0.25 to 0.25
- w_mix: float32 [2048], replicated, may hold values from -0.125 to 0.125
Outputs:
- mixed: bfloat16 [192, 2048], P('ep', 'tp')
- new_keys: bfloat16 [192, 4, 64], P('ep', 'tp')
- new_values: bfloat16 [192, 4, 64], P('ep', 'tp')
The draws below stay inside these ranges and needn't reach their ends.
Inputs may be any that keep to these rules, and one draw needn't show every extreme that they name: `routes`: the 2 experts of a row are distinct and lie in one group of 2 consecutive experts. Among the rows of one device each expert is named at most 12 times. One group, the same on every device, is named by exactly 12 rows of every device, so that each of its experts is named exactly 12 times by every device.
All inputs are finite; a program needn't handle non-finite values. No bound on the sum of `lengths` on one device may be relied on, other than what follows from the above.
Results may differ from the reference program's by a relative error of at most 0.019.
Values may be sent and summed in bfloat16 or wider, within the bound.
A program may use at most 128 MiB of HBM per device.

```python
import math
import jax
import jax.numpy as jnp
import numpy as np
from jax import lax

D = 2048
HEADS = 32
KV_HEADS = 4
DH = 64
FFE = 512
DENSE_FF = 8192
GROUPS = 4
TOP_K = 2
SEQ_DEV = 24
LEN = 1024
SEQUENCES = 192
EXPERTS = 8
EPG = 2
FULL_ROWS = 12
SLOTS = 96
N_TP = 4


def draw_routes(key, part):
    blocks = SEQUENCES // SEQ_DEV
    base_key = jax.random.fold_in(key, 11)
    full_key, blocks_key = jax.random.split(base_key)
    full_group = jax.random.randint(full_key, (), 0, GROUPS)

    def one_block(block_seed):
        ranking_key, other_key, tables_key = jax.random.split(block_seed, 3)
        ranking = jax.random.permutation(ranking_key, SEQ_DEV)
        other_group = jax.random.randint(other_key, (SEQ_DEV,), 1, GROUPS)
        group_ids = jnp.where(ranking < FULL_ROWS, full_group, (full_group + other_group) % GROUPS)
        same_group = group_ids[:, None] == group_ids[None, :]
        before = ranking[None, :] < ranking[:, None]
        position = jnp.sum(same_group & before, axis=1)
        tables = jax.vmap(lambda seed_key: jax.random.permutation(seed_key, EPG))(jax.random.split(tables_key, GROUPS))
        chosen = [tables[group_ids, (TOP_K * position + slot_index) % EPG] for slot_index in range(TOP_K)]
        return jnp.stack([group_ids * EPG + member for member in chosen], axis=1)
    result = jax.vmap(one_block)(jax.random.split(blocks_key, blocks))
    return result.reshape(SEQUENCES, TOP_K).astype(jnp.int32)


def shard_levels(rng, extent, pieces, low, top_value):
    loudness, own = 1.0, jax.random.fold_in(rng, 6)
    for dim, shards_of in pieces:
        draws = jnp.exp(jax.random.uniform(jax.random.fold_in(own, dim), (shards_of,), jnp.float32, low / len(pieces), top_value / len(pieces)))
        loudness = loudness * jnp.repeat(draws, extent[dim] // shards_of).reshape([-1 if axis == dim else 1 for axis in range(len(extent))])
    return loudness


def length_profile(number_of, total, reach, lean):
    portions = [(1 << 20) // math.isqrt(grade ** lean) + 1 for grade in range(2, number_of + 1)]
    surplus, counts = total - reach - (number_of - 1), [1] * (number_of - 1)
    while surplus > 0:
        candidates = [i for i in range(number_of - 1) if counts[i] < reach]
        whole, budget = sum([portions[i] for i in candidates]), surplus
        for i in candidates:
            more = min(reach - counts[i], max(1, budget * portions[i] // whole), surplus)
            counts[i] = counts[i] + more
            surplus = surplus - more
    return np.array([reach] + counts)


def uneven(rng, count, total, bound, slope):
    if count == 2:
        one = jax.random.randint(rng, (), max(1, total - bound), min(bound, total - 1) + 1)
        return jnp.stack([one, total - one])
    tallies = jnp.asarray(length_profile(count, total, bound, slope), jnp.int32)
    couples = (count - 1) // 2
    donor, sink = tallies[1:1 + 2 * couples:2], tallies[2:2 + 2 * couples:2]
    room = jnp.minimum(donor - 1, bound - sink)
    moved = jax.random.randint(jax.random.fold_in(rng, 1), (couples,), 0, 1 << 20) % (room + 1)
    tallies = tallies.at[1:1 + 2 * couples:2].set(donor - moved).at[2:2 + 2 * couples:2].set(sink + moved)
    return tallies[jax.random.permutation(jax.random.fold_in(rng, 2), count)]


def noise(key, dims, width, limit, pieces=(), kind=jnp.bfloat16):
    level = shard_levels(key, dims, pieces, -0.22, 0.18) if pieces else 1.0
    entries = jax.random.normal(key, dims, jnp.float32) * width * level
    return jnp.minimum(jnp.maximum(entries, -limit), limit).astype(kind)


def setup_inputs(seed: int = 0) -> dict:
    key_list = jax.random.split(jax.random.key(seed), 22)
    tokens = noise(key_list[0], (SEQUENCES, D), 1.0, 6.0, ((0, 8),))
    norm_attn = jnp.clip(1.0 + 0.18 * jax.random.normal(key_list[1], (D,), jnp.float32), 0.1, 1.9)
    w_query = noise(key_list[2], (D, HEADS * DH), D ** -0.5, 0.125, ((1, 4),))
    w_key = noise(key_list[3], (D, KV_HEADS * DH), D ** -0.5, 0.125, ((1, 4),))
    w_value = noise(key_list[4], (D, KV_HEADS * DH), D ** -0.5, 0.125, ((1, 4),))
    w_out = noise(key_list[5], (HEADS * DH, D), (HEADS * DH // 64) ** -0.5, 1.0, ((0, 4),))
    head_bias = jnp.clip(-7.0 + 4.0 * jax.random.uniform(key_list[6], (HEADS,), jnp.float32) ** shard_levels(key_list[6], (HEADS,), ((0, 4),), -0.2, 0.2), -7.0, -3.0)
    key_cache = noise(key_list[7], (SEQUENCES, KV_HEADS, LEN, DH), 1.0, 6.0, ((0, 8), (1, 4)))
    value_cache = noise(key_list[8], (SEQUENCES, KV_HEADS, LEN, DH), 1.0, 6.0, ((0, 8), (1, 4)))
    lengths = uneven(key_list[9], SEQUENCES, SEQUENCES * LEN // 2, LEN, 2).astype(jnp.int32)
    norm_ffn = jnp.clip(1.0 + 0.18 * jax.random.normal(key_list[10], (D,), jnp.float32), 0.1, 1.9)
    w_group = noise(key_list[11], (D, GROUPS), D ** -0.5, 0.125)
    w_fine = noise(key_list[12], (D, EXPERTS), D ** -0.5, 0.125)
    routes = draw_routes(jax.random.fold_in(key_list[21], 71), 0)
    e_gate = noise(key_list[14], (EXPERTS, D, FFE), D ** -0.5, 0.125, ((0, 8), (1, 4)))
    e_up = noise(key_list[15], (EXPERTS, D, FFE), D ** -0.5, 0.125, ((0, 8), (1, 4)))
    e_down = noise(key_list[16], (EXPERTS, FFE, D), (FFE // 16) ** -0.5, 1.0, ((0, 8), (2, 4)))
    d_gate = noise(key_list[17], (D, DENSE_FF), D ** -0.5, 0.125, ((0, 4), (1, 8)))
    d_up = noise(key_list[18], (D, DENSE_FF), D ** -0.5, 0.125, ((0, 4), (1, 8)))
    d_down = noise(key_list[19], (DENSE_FF, D), (DENSE_FF // 16) ** -0.5, 0.25, ((0, 8), (1, 4)))
    w_mix = noise(key_list[20], (D,), D ** -0.5, 0.125, (), jnp.float32)
    return dict(tokens=tokens, norm_attn=norm_attn, w_query=w_query, w_key=w_key, w_value=w_value, w_out=w_out, head_bias=head_bias, key_cache=key_cache, value_cache=value_cache, lengths=lengths, norm_ffn=norm_ffn, w_group=w_group, w_fine=w_fine, routes=routes, e_gate=e_gate, e_up=e_up, e_down=e_down, d_gate=d_gate, d_up=d_up, d_down=d_down, w_mix=w_mix)


def normed(values, gains):
    wide = values.astype(jnp.float32)
    return wide * lax.rsqrt(lax.optimization_barrier(jnp.mean(wide * wide, axis=-1, keepdims=True)) + 1e-06) * gains

def route_weights(group_logits, fine_logits, chosen, per_group):
    group_iota = lax.iota(jnp.int32, group_logits.shape[1])
    own_group = chosen[:, 0] // per_group
    own_logit = lax.optimization_barrier(jnp.sum(jnp.where(group_iota[None, :] == own_group[:, None], group_logits, 0.0), axis=1))
    group_share = 1.0 / lax.optimization_barrier(jnp.sum(jnp.exp(group_logits - own_logit[:, None]), axis=1))
    expert_iota = lax.iota(jnp.int32, fine_logits.shape[1])
    picked = lax.optimization_barrier(jnp.sum(jnp.where(expert_iota[None, None, :] == chosen[:, :, None], fine_logits[:, None, :], 0.0), axis=2))
    within = 1.0 / lax.optimization_barrier(jnp.sum(jnp.exp(picked[:, None, :] - picked[:, :, None]), axis=2))
    return group_share[:, None] * within

def attend(queries, key_cache, value_cache, lengths, head_bias):
    per_kv = HEADS // KV_HEADS
    query_blocks = queries.reshape(SEQUENCES // SEQ_DEV, SEQ_DEV, KV_HEADS, per_kv, DH)
    key_blocks = key_cache.reshape(SEQUENCES // SEQ_DEV, SEQ_DEV, KV_HEADS, LEN, DH)
    value_blocks = value_cache.reshape(SEQUENCES // SEQ_DEV, SEQ_DEV, KV_HEADS, LEN, DH)
    length_blocks = lengths.reshape(SEQUENCES // SEQ_DEV, SEQ_DEV)
    bias_table = head_bias.reshape(KV_HEADS, per_kv).astype(jnp.float32)

    def one_block(stacked):
        queries_b, keys_b, values_b, counts_b = stacked
        scores = jnp.einsum('bkgd,bksd->bkgs', queries_b.astype(jnp.float32), keys_b.astype(jnp.float32))
        scores = scores * DH ** (-0.5) + bias_table[None, :, :, None]
        positions = jnp.arange(LEN, dtype=jnp.int32)
        inside = (positions[None, :] < counts_b[:, None])[:, None, None, :]
        fails = jnp.where(inside, jax.nn.log_sigmoid(-scores), 0.0)
        between = lax.cumsum(fails, axis=3, reverse=True) - fails
        weights = jnp.where(inside, jnp.exp(jax.nn.log_sigmoid(scores) + between), 0.0).astype(jnp.bfloat16)
        mixed_b = jnp.einsum('bkgs,bksd->bkgd', weights.astype(jnp.float32), values_b.astype(jnp.float32))
        return mixed_b.astype(jnp.bfloat16)
    result = lax.map(one_block, (query_blocks, key_blocks, value_blocks, length_blocks))
    return result.reshape(SEQUENCES, HEADS * DH)

def reference(tokens, norm_attn, w_query, w_key, w_value, w_out, head_bias, key_cache, value_cache, lengths, norm_ffn, w_group, w_fine, routes, e_gate, e_up, e_down, d_gate, d_up, d_down, w_mix):
    h_first = normed(tokens, norm_attn).astype(jnp.bfloat16)
    queries = jnp.dot(h_first, w_query, preferred_element_type=jnp.float32).astype(jnp.bfloat16)
    new_keys = jnp.dot(h_first, w_key, preferred_element_type=jnp.float32).astype(jnp.bfloat16)
    new_values = jnp.dot(h_first, w_value, preferred_element_type=jnp.float32).astype(jnp.bfloat16)
    heads_out = attend(queries, key_cache, value_cache, lengths, head_bias)
    per_tp = HEADS * DH // N_TP
    attended = jnp.zeros((SEQUENCES, D), jnp.float32)
    for block_index in range(N_TP):
        piece = jnp.dot(heads_out[:, block_index * per_tp:(block_index + 1) * per_tp], w_out[block_index * per_tp:(block_index + 1) * per_tp], preferred_element_type=jnp.float32).astype(jnp.bfloat16)
        attended = attended + lax.optimization_barrier(piece).astype(jnp.float32)
    resid = tokens.astype(jnp.float32) + attended
    h_second = normed(resid, norm_ffn).astype(jnp.bfloat16)
    group_logits = jnp.dot(h_second, w_group, preferred_element_type=jnp.float32)
    fine_logits = jnp.dot(h_second, w_fine, preferred_element_type=jnp.float32)
    shares = route_weights(group_logits, fine_logits, routes, EPG)

    def expert_step(totals, stacked):
        gate_w, up_w, down_w, number = stacked
        names_it = routes == number
        is_hit = jnp.any(names_it, axis=1)
        expert_share = lax.optimization_barrier(jnp.sum(jnp.where(names_it, shares, 0.0), axis=1))
        row_index = jnp.nonzero(is_hit, size=SLOTS, fill_value=0)[0].astype(jnp.int32)
        is_valid = (jnp.arange(SLOTS, dtype=jnp.int32) < jnp.sum(is_hit.astype(jnp.int32))).astype(jnp.float32)
        picked_rows = h_second[row_index]
        gate_pre = jnp.dot(picked_rows, gate_w, preferred_element_type=jnp.float32)
        up_pre = jnp.dot(picked_rows, up_w, preferred_element_type=jnp.float32)
        hidden = (jax.nn.silu(gate_pre) * up_pre).astype(jnp.bfloat16)
        expert_out = jnp.dot(hidden, down_w, preferred_element_type=jnp.float32).astype(jnp.bfloat16)
        scaled = expert_out.astype(jnp.float32) * (expert_share[row_index] * is_valid)[:, None]
        return (totals.at[row_index].add(scaled), None)
    moe, _ = lax.scan(expert_step, jnp.zeros((SEQUENCES, D), jnp.float32), (e_gate, e_up, e_down, jnp.arange(EXPERTS, dtype=jnp.int32)))
    dense_gate = jnp.dot(h_second, d_gate, preferred_element_type=jnp.float32)
    dense_up = jnp.dot(h_second, d_up, preferred_element_type=jnp.float32)
    dense_hidden = (jax.nn.silu(dense_gate) * dense_up).astype(jnp.bfloat16)
    dense = jnp.dot(dense_hidden, d_down, preferred_element_type=jnp.float32)
    mix_gate = jax.nn.sigmoid(jnp.dot(h_second.astype(jnp.float32), w_mix, precision=lax.Precision.HIGHEST))
    mixed = (resid + moe + mix_gate[:, None] * dense).astype(jnp.bfloat16)
    return (mixed, new_keys.reshape(SEQUENCES, KV_HEADS, DH), new_values.reshape(SEQUENCES, KV_HEADS, DH))
```

```python
import jax
import jax.numpy as jnp
from jax import lax
from jax.experimental import pallas as pl
from jax.experimental.pallas import tpu as pltpu
from jax.sharding import PartitionSpec as P
import functools

GROUPS = 4
TOP_K = 2


norm_eps = 1e-06
segment_len = 128


def normed(values, gains):
    wide = values.astype(jnp.float32)
    return wide * lax.rsqrt(jnp.mean(wide * wide, axis=-1, keepdims=True) + norm_eps) * gains


def suffix_sums(terms):
    length = terms.shape[-1]
    pieces = length // segment_len
    shaped = terms.reshape(terms.shape[:-1] + (pieces, segment_len))
    inner = lax.iota(jnp.int32, segment_len)
    later_inner = (inner[:, None] > inner[None, :]).astype(jnp.float32)
    within = jnp.einsum("...ij,jk->...ik", shaped, later_inner, precision=lax.Precision.HIGHEST)
    outer = lax.iota(jnp.int32, pieces)
    later_outer = (outer[:, None] > outer[None, :]).astype(jnp.float32)
    carried = jnp.einsum(
        "...i,ij->...j", jnp.sum(shaped, axis=-1), later_outer, precision=lax.Precision.HIGHEST
    )
    return (within + carried[..., None]).reshape(terms.shape)


def stick_read(queries, keys, values, lengths, bias_table):
    scores = jnp.einsum("bkgd,bksd->bkgs", queries, keys, preferred_element_type=jnp.float32)
    scores = scores * queries.shape[-1] ** (-0.5) + bias_table[None, :, :, None]
    positions = lax.iota(jnp.int32, keys.shape[2])
    inside = (positions[None, :] < lengths[:, None])[:, None, None, :]
    fails = jnp.where(inside, jax.nn.log_sigmoid(-scores), 0.0)
    weights = jnp.where(inside, jnp.exp(jax.nn.log_sigmoid(scores) + suffix_sums(fails)), 0.0)
    result = jnp.einsum(
        "bkgs,bksd->bkgd", weights.astype(jnp.bfloat16), values, preferred_element_type=jnp.float32
    )
    return result.astype(jnp.bfloat16).reshape(queries.shape[0], -1)


LANES = 128
MESH = pl.DeviceIdType.MESH


def tail_kernel(
    dims,
    partial_ref, tokens_ref, gain_ref, routes_ref, aux_w_ref,
    dg_hbm, du_hbm, dd_hbm, eg_hbm, eu_hbm, ed_hbm,
    out_ref,
    dg, du, dd, eg, eu, ed,
    route_buf, tp_buf, resid_buf, rows_buf, pick_buf, mask_buf, chosen_buf,
    dsend, drecv, esend, erecv, asend, arecv,
    hid_buf, ehid_buf, dense_buf, eout_buf, fin_send, fin_recv,
    load_sem, rt_s, rt_r, tp_s, tp_r, row_s, row_r, pre_s, pre_r, hid_s, hid_r, fin_s, fin_r,
):
    E, T, S, W, U, F, slots, per_group, fine_count = dims
    ET = E // T
    RB, CB = ET * S, ET * slots
    me_e, me_t = lax.axis_index("ep"), lax.axis_index("tp")

    loads = [
        pltpu.make_async_copy(src, dst, load_sem.at[i])
        for i, (src, dst) in enumerate(
            [(dg_hbm, dg), (du_hbm, du), (eg_hbm, eg), (eu_hbm, eu), (dd_hbm, dd), (ed_hbm, ed)]
        )
    ]
    for load in loads:
        load.start()

    barrier = pltpu.get_barrier_semaphore()

    def greet(d, carry):
        pl.semaphore_signal(
            barrier, inc=1, device_id={"ep": lax.rem(me_e + d, E)}, device_id_type=MESH
        )
        return carry

    lax.fori_loop(1, E, greet, 0)
    for j in range(1, T):
        pl.semaphore_signal(
            barrier, inc=1, device_id={"tp": lax.rem(me_t + j, T)}, device_id_type=MESH
        )
    pl.semaphore_wait(barrier, E - 1 + T - 1)

    def remote(src, dst, send, recv, device):
        return pltpu.make_async_remote_copy(
            src_ref=src, dst_ref=dst, send_sem=send, recv_sem=recv,
            device_id=device, device_id_type=MESH,
        )

    def feature_block(index):
        return pl.ds(pl.multiple_of(index * W, LANES), W)

    tp_copies = []
    for j in range(1, T):
        peer = lax.rem(me_t + j, T)
        tp_copies.append(
            remote(
                partial_ref.at[:, feature_block(peer)], tp_buf.at[j - 1],
                tp_s.at[j - 1], tp_r.at[j - 1], {"tp": peer},
            )
        )
        tp_copies[-1].start()

    def route_copy(d):
        return remote(
            routes_ref, route_buf.at[d], rt_s.at[d], rt_r.at[d], {"ep": lax.rem(me_e + d, E)}
        )

    def row_copy(d):
        return remote(
            rows_buf.at[0], rows_buf.at[d], row_s.at[d], row_r.at[d], {"ep": lax.rem(me_e + d, E)}
        )

    def fin_copy(d):
        return remote(
            fin_send.at[d], fin_recv.at[d], fin_s.at[d], fin_r.at[d],
            {"ep": lax.rem(me_e - d + E, E)},
        )

    def each(first, body):
        def step(d, carry):
            body(d)
            return carry

        lax.fori_loop(first, E, step, 0)

    each(1, lambda d: route_copy(d).start())
    route_buf[0] = routes_ref[...]

    gain = gain_ref[:, feature_block(me_t)]
    total = tokens_ref[:, feature_block(me_t)].astype(jnp.float32)
    total = total + partial_ref[:, feature_block(me_t)].astype(jnp.float32)
    for j in range(1, T):
        tp_copies[j - 1].wait_recv()
        total = total + tp_buf[j - 1].astype(jnp.float32)
    resid_buf[...] = total
    rows_buf[0] = (total * gain).astype(jnp.bfloat16)
    each(1, lambda d: row_copy(d).start())

    each(1, lambda d: route_copy(d).wait_recv())
    own = me_e.astype(jnp.float32)
    before = (
        lax.broadcasted_iota(jnp.int32, (LANES, LANES), 0)
        < lax.broadcasted_iota(jnp.int32, (LANES, LANES), 1)
    ).astype(jnp.float32).astype(jnp.bfloat16)
    slot_iota = lax.broadcasted_iota(jnp.int32, (slots, LANES), 0).astype(jnp.float32)
    lane_iota = lax.broadcasted_iota(jnp.int32, (slots, LANES), 1).astype(jnp.float32)

    def pick(d):
        named = route_buf[d]
        hits = jnp.where(named == own, 1.0, 0.0)
        ranks = jnp.dot(hits.astype(jnp.bfloat16), before, preferred_element_type=jnp.float32)
        rank = jnp.sum(ranks, axis=0, keepdims=True)
        hit = jnp.sum(hits, axis=0, keepdims=True)
        picks = jnp.where(slot_iota == rank, 1.0, 0.0) * hit
        pick_buf[d] = picks
        mask = jnp.zeros((slots, LANES), jnp.float32)
        for i in range(TOP_K):
            chosen = jnp.sum(picks * named[i : i + 1, :], axis=1, keepdims=True)
            mask = jnp.where(lane_iota == chosen + float(GROUPS), 1.0, mask)
        mask_buf[d] = mask

    each(0, pick)

    def gather(d):
        chosen_buf[d] = jnp.dot(
            pick_buf[d][:, :S].astype(jnp.bfloat16), rows_buf[d],
            preferred_element_type=jnp.float32,
        )

    gather(0)

    def gather_arrived(d):
        row_copy(d).wait_recv()
        gather(d)

    each(1, gather_arrived)
    for load in loads[:4]:
        load.wait()

    inverse = 1.0 / gain
    aux_w = aux_w_ref[me_t]

    def dot(a, b):
        return jnp.dot(a, b, preferred_element_type=jnp.float32)

    def partials(owner):
        rows = rows_buf[pl.ds(owner * ET, ET)].astype(jnp.float32).reshape(RB, W)
        picked = chosen_buf[pl.ds(owner * ET, ET)].reshape(CB, W)
        both = jnp.concatenate([rows, picked], axis=0)
        scaled = both * inverse
        squares = jnp.sum(scaled * scaled, axis=1, keepdims=True)
        rows, picked = rows.astype(jnp.bfloat16), picked.astype(jnp.bfloat16)
        lanes = lax.broadcasted_iota(jnp.int32, (RB + CB, LANES), 1)
        aux = dot(both.astype(jnp.bfloat16), aux_w) + jnp.where(lanes == LANES - 1, squares, 0.0)
        return rows, picked, aux

    pre_copies = []
    for j in range(1, T):
        owner = lax.rem(me_t + j, T)
        rows, picked, aux = partials(owner)
        dsend[j - 1, :, :U] = dot(rows, dg[...]).astype(jnp.bfloat16)
        dsend[j - 1, :, U:] = dot(rows, du[...]).astype(jnp.bfloat16)
        esend[j - 1, :, :F] = dot(picked, eg[...]).astype(jnp.bfloat16)
        esend[j - 1, :, F:] = dot(picked, eu[...]).astype(jnp.bfloat16)
        asend[j - 1] = aux
        for k, (src, dst) in enumerate([(dsend, drecv), (esend, erecv), (asend, arecv)]):
            copy = remote(
                src.at[j - 1], dst.at[j - 1], pre_s.at[j - 1, k], pre_r.at[j - 1, k], {"tp": owner}
            )
            copy.start()
            pre_copies.append(copy)
    rows, picked, aux = partials(me_t)
    gate, up = dot(rows, dg[...]), dot(rows, du[...])
    egate, eup = dot(picked, eg[...]), dot(picked, eu[...])
    for copy in pre_copies:
        copy.wait_recv()
    for j in range(T - 1):
        aux = aux + arecv[j]
        gate = gate + drecv[j, :, :U].astype(jnp.float32)
        up = up + drecv[j, :, U:].astype(jnp.float32)
        egate = egate + erecv[j, :, :F].astype(jnp.float32)
        eup = eup + erecv[j, :, F:].astype(jnp.float32)
    scale = lax.rsqrt(aux[:, LANES - 1 :] / (T * W) + norm_eps)
    logits = aux * scale
    mix = GROUPS + fine_count
    mix_gate = jax.nn.sigmoid(logits[:RB, mix : mix + 1] + logits[:RB, mix + 1 : mix + 2])
    dense_scale, slot_scale = scale[:RB], scale[RB:]
    gate, up = gate * dense_scale, up * dense_scale
    hid_buf[me_t] = (jax.nn.silu(gate) * up * mix_gate).astype(jnp.bfloat16)

    slot_logits = logits[RB:]
    lanes = lax.broadcasted_iota(jnp.int32, (CB, LANES), 1)

    def at_lane(lane):
        return jnp.sum(jnp.where(lanes == lane, slot_logits, 0.0), axis=1, keepdims=True)

    own_group, own_fine = at_lane(me_e // per_group), at_lane(me_e + GROUPS)
    named = mask_buf[pl.ds(me_t * ET, ET)].reshape(CB, LANES)

    def share(inside, own_logit):
        terms = jnp.exp(jnp.where(inside, slot_logits - own_logit, -jnp.inf))
        return 1.0 / jnp.sum(terms, axis=1, keepdims=True)

    shares = share(lanes < GROUPS, own_group) * share(
        (named > 0.0) | (lanes == me_e + GROUPS), own_fine
    )
    egate, eup = egate * slot_scale, eup * slot_scale
    ehid_buf[me_t] = (jax.nn.silu(egate) * eup * shares).astype(jnp.bfloat16)

    hid_copies = []
    for j in range(1, T):
        for k, buf in enumerate([hid_buf, ehid_buf]):
            copy = remote(
                buf.at[me_t], buf.at[me_t], hid_s.at[j - 1, k], hid_r.at[j - 1, k],
                {"tp": lax.rem(me_t + j, T)},
            )
            copy.start()
            hid_copies.append(copy)
    for load in loads[4:]:
        load.wait()
    for copy in hid_copies:
        copy.wait_recv()

    dense_buf[...] = dot(hid_buf[...].reshape(E * S, U), dd[...]).reshape(E, S, W)
    eout_buf[...] = dot(ehid_buf[...].reshape(E * slots, F), ed[...]).reshape(E, slots, W)

    def output_of(d):
        back = pick_buf[d].T[:S].astype(jnp.bfloat16)
        return dense_buf[d] + dot(back, eout_buf[d].astype(jnp.bfloat16))

    def finish(d):
        fin_send[d] = output_of(d).astype(jnp.bfloat16)
        fin_copy(d).start()

    each(1, finish)
    resid_buf[...] += output_of(0)

    def collect(d):
        fin_copy(d).wait_recv()
        resid_buf[...] += fin_recv[d].astype(jnp.float32)

    each(1, collect)
    out_ref[...] = resid_buf[...].astype(jnp.bfloat16)

    for copy in tp_copies + pre_copies + hid_copies:
        copy.wait_send()
    each(1, lambda d: route_copy(d).wait_send())
    each(1, lambda d: row_copy(d).wait_send())
    each(1, lambda d: fin_copy(d).wait_send())


def tail(partial, tokens, gain, routes, w_group, w_fine, w_mix, dg, du, dd, eg, eu, ed):
    E, T = lax.axis_size("ep"), lax.axis_size("tp")
    S, D = tokens.shape
    W, U = dg.shape
    F = eg.shape[1]
    per_group = E // GROUPS
    capacity = max(2, (S + per_group - 1) // per_group)
    slots = (capacity + 7) // 8 * 8
    ET = E // T
    RB, CB = ET * S, ET * slots
    high = lax.reduce_precision(w_mix, 8, 7)
    aux_w = jnp.concatenate(
        [w_group, w_fine, high.astype(jnp.bfloat16)[:, None],
         (w_mix - high).astype(jnp.bfloat16)[:, None]], axis=1,
    )
    aux_w = jnp.pad(aux_w, ((0, 0), (0, LANES - aux_w.shape[1]))).reshape(T, W, LANES)
    route_rows = jnp.pad(
        routes.T.astype(jnp.float32), ((0, 8 - TOP_K), (0, LANES - S)), constant_values=-1.0
    )
    bf16, f32 = jnp.bfloat16, jnp.float32
    vmem = pl.BlockSpec(memory_space=pltpu.VMEM)
    anywhere = pl.BlockSpec(memory_space=pl.ANY)
    dma = pltpu.SemaphoreType.DMA
    dims = (E, T, S, W, U, F, slots, per_group, w_fine.shape[1])
    return pl.pallas_call(
        functools.partial(tail_kernel, dims),
        out_shape=jax.ShapeDtypeStruct((S, W), bf16),
        in_specs=[vmem] * 5 + [anywhere] * 6,
        out_specs=vmem,
        scratch_shapes=[
            pltpu.VMEM((W, U), bf16), pltpu.VMEM((W, U), bf16), pltpu.VMEM((U, W), bf16),
            pltpu.VMEM((W, F), bf16), pltpu.VMEM((W, F), bf16), pltpu.VMEM((F, W), bf16),
            pltpu.VMEM((E, 8, LANES), f32),
            pltpu.VMEM((T - 1, S, W), bf16),
            pltpu.VMEM((S, W), f32),
            pltpu.VMEM((E, S, W), bf16),
            pltpu.VMEM((E, slots, LANES), f32),
            pltpu.VMEM((E, slots, LANES), f32),
            pltpu.VMEM((E, slots, W), f32),
            pltpu.VMEM((T - 1, RB, 2 * U), bf16), pltpu.VMEM((T - 1, RB, 2 * U), bf16),
            pltpu.VMEM((T - 1, CB, 2 * F), bf16), pltpu.VMEM((T - 1, CB, 2 * F), bf16),
            pltpu.VMEM((T - 1, RB + CB, LANES), f32), pltpu.VMEM((T - 1, RB + CB, LANES), f32),
            pltpu.VMEM((T, RB, U), bf16), pltpu.VMEM((T, CB, F), bf16),
            pltpu.VMEM((E, S, W), f32), pltpu.VMEM((E, slots, W), f32),
            pltpu.VMEM((E, S, W), bf16), pltpu.VMEM((E, S, W), bf16),
            dma((6,)), dma((E,)), dma((E,)), dma((T - 1,)), dma((T - 1,)), dma((E,)), dma((E,)),
            dma((T - 1, 3)), dma((T - 1, 3)), dma((T - 1, 2)), dma((T - 1, 2)),
            dma((E,)), dma((E,)),
        ],
        compiler_params=pltpu.CompilerParams(
            collective_id=0, has_side_effects=True, vmem_limit_bytes=48 * 1024 * 1024
        ),
        name="tail",
    )(partial, tokens, gain[None, :], route_rows, aux_w, dg, du, dd, eg, eu, ed)


def shards(
    tokens,
    norm_attn,
    w_query,
    w_key,
    w_value,
    w_out,
    head_bias,
    key_cache,
    value_cache,
    lengths,
    norm_ffn,
    w_group,
    w_fine,
    routes,
    e_gate,
    e_up,
    e_down,
    d_gate,
    d_up,
    d_down,
    w_mix,
):
    seq_count = tokens.shape[0]
    kv_local = key_cache.shape[1]
    head_dim = key_cache.shape[3]
    h_first = normed(tokens, norm_attn).astype(jnp.bfloat16)
    queries = jnp.dot(h_first, w_query, preferred_element_type=jnp.float32).astype(jnp.bfloat16)
    new_keys = jnp.dot(h_first, w_key, preferred_element_type=jnp.float32).astype(jnp.bfloat16)
    new_values = jnp.dot(h_first, w_value, preferred_element_type=jnp.float32).astype(jnp.bfloat16)
    grouped = queries.reshape(seq_count, kv_local, -1, head_dim)
    heads_out = stick_read(
        grouped, key_cache, value_cache, lengths, head_bias.reshape(kv_local, -1)
    )
    partial_value = jnp.dot(heads_out, w_out, preferred_element_type=jnp.float32).astype(
        jnp.bfloat16
    )
    mixed = tail(
        partial_value, tokens, norm_ffn, routes, w_group, w_fine, w_mix,
        d_gate, d_up, d_down, e_gate[0], e_up[0], e_down[0],
    )
    return (
        mixed,
        new_keys.reshape(seq_count, kv_local, head_dim),
        new_values.reshape(seq_count, kv_local, head_dim),
    )


def solution(mesh):
    placed = (
        P("ep", None),
        P(),
        P(None, "tp"),
        P(None, "tp"),
        P(None, "tp"),
        P("tp", None),
        P("tp"),
        P("ep", "tp", None, None),
        P("ep", "tp", None, None),
        P("ep"),
        P(),
        P(),
        P(),
        P("ep", None),
        P("ep", "tp", None),
        P("ep", "tp", None),
        P("ep", None, "tp"),
        P("tp", "ep"),
        P("tp", "ep"),
        P("ep", "tp"),
        P(),
    )
    return jax.shard_map(
        shards,
        mesh=mesh,
        in_specs=placed,
        out_specs=(P("ep", "tp"), P("ep", "tp", None), P("ep", "tp", None)),
        check_vma=False,
    )
```

```python
import jax
import jax.numpy as jnp
from jax import lax
from jax.experimental import pallas as pl
from jax.experimental.pallas import tpu as pltpu
from jax.sharding import PartitionSpec as P
import functools

GROUPS = 4
TOP_K = 2


norm_eps = 1e-06


def normed(values, gains):
    wide = values.astype(jnp.float32)
    return wide * lax.rsqrt(jnp.mean(wide * wide, axis=-1, keepdims=True) + norm_eps) * gains


def stick_kernel(batch, heads, lengths_ref, bias_ref, q_ref, k_ref, v_ref, out_ref):
    step = pl.program_id(0)
    head_dim, length = k_ref.shape[1:]
    pieces = length // LANES
    rows = batch * heads
    head = lax.broadcasted_iota(jnp.int32, (heads, length), 0)
    position = lax.broadcasted_iota(jnp.int32, (heads, length), 1)
    bias = jnp.zeros((heads, length), jnp.float32)
    for h in range(heads):
        bias = jnp.where(head == h, bias_ref[h], bias)
    parts, insides = [], []
    for i in range(batch):
        product = jnp.dot(q_ref[i], k_ref[i], preferred_element_type=jnp.float32)
        parts.append(product * head_dim ** (-0.5) + bias)
        insides.append((position < lengths_ref[step * batch + i]).astype(jnp.float32))
    scores = jnp.concatenate(parts, axis=0)
    inside = jnp.concatenate(insides, axis=0) > 0.0
    log_fail = -(jnp.maximum(scores, 0.0) + jnp.log1p(jnp.exp(-jnp.abs(scores))))
    fails = jnp.where(inside, log_fail, 0.0)
    stacked = jnp.concatenate(
        [fails[:, p * LANES : (p + 1) * LANES] for p in range(pieces)], axis=0
    )
    later = (
        lax.broadcasted_iota(jnp.int32, (LANES, LANES), 0)
        > lax.broadcasted_iota(jnp.int32, (LANES, LANES), 1)
    ).astype(jnp.float32).astype(jnp.bfloat16)
    within, left = jnp.zeros_like(stacked), stacked
    for _ in range(3):
        part = left.astype(jnp.bfloat16)
        left = left - part.astype(jnp.float32)
        within = within + jnp.dot(part, later, preferred_element_type=jnp.float32)
    totals = jnp.sum(stacked, axis=1, keepdims=True)
    carry, sums = jnp.zeros((rows, 1), jnp.float32), [None] * pieces
    for p in reversed(range(pieces)):
        sums[p] = within[p * rows : (p + 1) * rows] + carry
        carry = carry + totals[p * rows : (p + 1) * rows]
    suffix = jnp.concatenate(sums, axis=1)
    stick = jnp.where(inside, jnp.exp(scores + log_fail + suffix), 0.0)
    for i in range(batch):
        out_ref[i] = lax.dot_general(
            stick[i * heads : (i + 1) * heads].astype(jnp.bfloat16), v_ref[i],
            (((1,), (1,)), ((), ())), preferred_element_type=jnp.float32,
        ).astype(jnp.bfloat16)


def stick_read(queries, keys, values, lengths, bias):
    count, heads, head_dim = queries.shape
    length = keys.shape[2]
    batch = next(b for b in (4, 3, 2, 1) if count % b == 0)
    smem = pl.BlockSpec(memory_space=pltpu.SMEM)
    cache = pl.BlockSpec((batch, head_dim, length), lambda i: (i, 0, 0))
    small = pl.BlockSpec((batch, heads, head_dim), lambda i: (i, 0, 0))
    return pl.pallas_call(
        functools.partial(stick_kernel, batch, heads),
        grid=(count // batch,),
        out_shape=jax.ShapeDtypeStruct(queries.shape, jnp.bfloat16),
        in_specs=[smem, smem, small, cache, cache],
        out_specs=small,
        cost_estimate=pl.CostEstimate(
            flops=4 * count * heads * head_dim * length,
            bytes_accessed=4 * count * head_dim * length,
            transcendentals=3 * count * heads * length,
        ),
        name="stick",
    )(lengths, bias, queries, keys, values).reshape(count, -1)


LANES = 128
MESH = pl.DeviceIdType.MESH


def tail_kernel(
    dims,
    partial_ref, tokens_ref, first_gain_ref, gain_ref, routes_ref, group_ref, fine_ref, mix_ref,
    dg_hbm, du_hbm, dd_hbm, eg_hbm, eu_hbm, ed_hbm, key_hbm, value_hbm,
    out_ref, key_out, value_out,
    dg, du, dd, eg, eu, ed, key_w, value_w, aux_w,
    route_buf, tp_buf, resid_buf, rows_buf, pick_buf, mask_buf, chosen_buf,
    gsend, grecv, usend, urecv, esend, erecv, asend, arecv,
    hid_buf, ehid_buf, dense_buf, eout_buf, fin_send, fin_recv,
    load_sem, rt_s, rt_r, tp_s, tp_r, row_s, row_r, pre_s, pre_r, hid_s, hid_r, fin_s, fin_r,
):
    E, T, S, W, U, F, slots, per_group, fine_count = dims
    ET = E // T
    RB, CB = ET * S, ET * slots
    me_e, me_t = lax.axis_index("ep"), lax.axis_index("tp")

    loads = [
        pltpu.make_async_copy(src, dst, load_sem.at[i])
        for i, (src, dst) in enumerate(
            [(dg_hbm, dg), (du_hbm, du), (eg_hbm, eg), (eu_hbm, eu), (dd_hbm, dd), (ed_hbm, ed),
             (key_hbm, key_w), (value_hbm, value_w)]
        )
    ]
    for load in loads:
        load.start()

    feature_rows = pl.ds(pl.multiple_of(me_t * W, LANES), W)
    fine_at = 16
    mix = fine_at + (fine_count + 15) // 16 * 16
    mix_w = mix_ref[:, feature_rows]
    high = mix_w.astype(jnp.bfloat16)
    aux_w[...] = jnp.zeros_like(aux_w)
    aux_w[:GROUPS] = group_ref[:, feature_rows]
    aux_w[fine_at : fine_at + fine_count] = fine_ref[:, feature_rows]
    aux_w[mix : mix + 1] = high
    aux_w[mix + 16 : mix + 17] = (mix_w - high.astype(jnp.float32)).astype(jnp.bfloat16)
    route_buf[0] = jnp.full((8, LANES), -1.0, jnp.float32)
    route_buf[0, :TOP_K, :S] = routes_ref[...].astype(jnp.float32)

    barrier = pltpu.get_barrier_semaphore()

    def greet(d, carry):
        pl.semaphore_signal(
            barrier, inc=1, device_id={"ep": lax.rem(me_e + d, E)}, device_id_type=MESH
        )
        return carry

    lax.fori_loop(1, E, greet, 0)
    for j in range(1, T):
        pl.semaphore_signal(
            barrier, inc=1, device_id={"tp": lax.rem(me_t + j, T)}, device_id_type=MESH
        )
    pl.semaphore_wait(barrier, E - 1 + T - 1)

    def remote(src, dst, send, recv, device):
        return pltpu.make_async_remote_copy(
            src_ref=src, dst_ref=dst, send_sem=send, recv_sem=recv,
            device_id=device, device_id_type=MESH,
        )

    def feature_block(index):
        return pl.ds(pl.multiple_of(index * W, LANES), W)

    tp_copies = []
    for j in range(1, T):
        peer = lax.rem(me_t + j, T)
        tp_copies.append(
            remote(
                partial_ref.at[:, feature_block(peer)], tp_buf.at[j - 1],
                tp_s.at[j - 1], tp_r.at[j - 1], {"tp": peer},
            )
        )
        tp_copies[-1].start()

    def route_copy(d):
        return remote(
            route_buf.at[0], route_buf.at[d], rt_s.at[d], rt_r.at[d], {"ep": lax.rem(me_e + d, E)}
        )

    def row_copy(d):
        return remote(
            rows_buf.at[0], rows_buf.at[d], row_s.at[d], row_r.at[d], {"ep": lax.rem(me_e + d, E)}
        )

    def fin_copy(d):
        return remote(
            fin_send.at[d], fin_recv.at[d], fin_s.at[d], fin_r.at[d],
            {"ep": lax.rem(me_e - d + E, E)},
        )

    def each(first, body):
        def step(d, carry):
            body(d)
            return carry

        lax.fori_loop(first, E, step, 0)

    each(1, lambda d: route_copy(d).start())

    def dot(a, b):
        return jnp.dot(a, b, preferred_element_type=jnp.float32)

    def dot_t(a, b):
        return lax.dot_general(
            a, b, (((1,), (1,)), ((), ())), preferred_element_type=jnp.float32
        )

    for load in loads[6:]:
        load.wait()
    h_first = normed(tokens_ref[...], first_gain_ref[...]).astype(jnp.bfloat16)
    key_out[...] = dot_t(h_first, key_w[...]).astype(jnp.bfloat16)
    value_out[...] = dot_t(h_first, value_w[...]).astype(jnp.bfloat16)

    gain = gain_ref[:, feature_block(me_t)]
    total = tokens_ref[:, feature_block(me_t)].astype(jnp.float32)
    total = total + partial_ref[:, feature_block(me_t)].astype(jnp.float32)
    for j in range(1, T):
        tp_copies[j - 1].wait_recv()
        total = total + tp_buf[j - 1].astype(jnp.float32)
    resid_buf[...] = total
    rows_buf[0] = (total * gain).astype(jnp.bfloat16)

    partner = me_t + 1 - 2 * lax.rem(me_t, 2)
    across = lax.rem(me_t + T // 2, T)
    opposite = lax.rem(partner + T // 2, T)

    def block_of(owner, body):
        def step(i, carry):
            body(owner * ET + i)
            return carry

        lax.fori_loop(0, ET, step, 0)

    def from_others(body):
        def guarded(d):
            @pl.when(d > 0)
            def _():
                body(d)

        return guarded

    for owner in (opposite, across, partner, me_t):
        block_of(owner, from_others(lambda d: row_copy(d).start()))

    each(1, lambda d: route_copy(d).wait_recv())
    own = me_e.astype(jnp.float32)
    before = (
        lax.broadcasted_iota(jnp.int32, (LANES, LANES), 0)
        < lax.broadcasted_iota(jnp.int32, (LANES, LANES), 1)
    ).astype(jnp.float32).astype(jnp.bfloat16)
    slot_iota = lax.broadcasted_iota(jnp.int32, (slots, LANES), 0).astype(jnp.float32)
    lane_iota = lax.broadcasted_iota(jnp.int32, (slots, LANES), 1).astype(jnp.float32)

    def pick(d):
        named = route_buf[d]
        hits = jnp.where(named == own, 1.0, 0.0)
        ranks = jnp.dot(hits.astype(jnp.bfloat16), before, preferred_element_type=jnp.float32)
        rank = jnp.sum(ranks, axis=0, keepdims=True)
        hit = jnp.sum(hits, axis=0, keepdims=True)
        picks = jnp.where(slot_iota == rank, 1.0, 0.0) * hit
        pick_buf[d] = picks
        mask = jnp.zeros((slots, LANES), jnp.float32)
        for i in range(TOP_K):
            chosen = jnp.sum(picks * named[i : i + 1, :], axis=1, keepdims=True)
            mask = jnp.where(lane_iota == chosen + float(fine_at), 1.0, mask)
        mask_buf[d] = mask

    each(0, pick)

    def gather(d):
        chosen_buf[d] = jnp.dot(
            pick_buf[d][:, :S].astype(jnp.bfloat16), rows_buf[d],
            preferred_element_type=jnp.float32,
        )

    def gather_arrived(d):
        @pl.when(d > 0)
        def _():
            row_copy(d).wait_recv()

        gather(d)

    for load in loads[:4]:
        load.wait()

    inverse = 1.0 / gain

    def partials(owner):
        block_of(owner, gather_arrived)
        rows = rows_buf[pl.ds(owner * ET, ET)].astype(jnp.float32).reshape(RB, W)
        picked = chosen_buf[pl.ds(owner * ET, ET)].reshape(CB, W)
        both = jnp.concatenate([rows, picked], axis=0)
        scaled = both * inverse
        squares = jnp.sum(scaled * scaled, axis=1, keepdims=True)
        rows, picked = rows.astype(jnp.bfloat16), picked.astype(jnp.bfloat16)
        lanes = lax.broadcasted_iota(jnp.int32, (RB + CB, LANES), 1)
        aux = dot_t(both.astype(jnp.bfloat16), aux_w[...]) + jnp.where(lanes == LANES - 1, squares, 0.0)
        return rows, picked, aux

    pairs = [(gsend, grecv), (usend, urecv), (esend, erecv), (asend, arecv)]
    pre_copies = {}

    def send(n, k, value, device):
        src, dst = pairs[k]
        src[n] = value.astype(src.dtype)
        pre_copies[n, k] = remote(
            src.at[n], dst.at[n], pre_s.at[n, k], pre_r.at[n, k], {"tp": device}
        )
        pre_copies[n, k].start()

    def products(owner, consume):
        rows, picked, aux = partials(owner)
        consume(0, dot(rows, dg[...]))
        consume(1, dot(rows, du[...]))
        consume(2, jnp.concatenate([dot(picked, eg[...]), dot(picked, eu[...])], axis=1))
        consume(3, aux)

    def arrived(n, k):
        pre_copies[n, k].wait_recv()
        return pairs[k][1][n].astype(jnp.float32)

    products(opposite, lambda k, value: send(0, k, value, partner))
    products(across, lambda k, value: send(1, k, value + arrived(0, k), across))
    products(partner, lambda k, value: send(2, k, value, partner))
    kept = {}

    def keep(k, value):
        kept[k] = value + arrived(2, k)

    products(me_t, keep)
    gate, up, both_e, aux = [kept[k] + arrived(1, k) for k in range(4)]
    egate, eup = both_e[:, :F], both_e[:, F:]
    scale = lax.rsqrt(aux[:, LANES - 1 :] / (T * W) + norm_eps)
    logits = aux * scale
    mix_gate = jax.nn.sigmoid(logits[:RB, mix : mix + 1] + logits[:RB, mix + 16 : mix + 17])
    dense_scale, slot_scale = scale[:RB], scale[RB:]
    gate, up = gate * dense_scale, up * dense_scale
    hid_buf[me_t] = (jax.nn.silu(gate) * up * mix_gate).astype(jnp.bfloat16)

    slot_logits = logits[RB:]
    lanes = lax.broadcasted_iota(jnp.int32, (CB, LANES), 1)

    def at_lane(lane):
        return jnp.sum(jnp.where(lanes == lane, slot_logits, 0.0), axis=1, keepdims=True)

    own_group, own_fine = at_lane(me_e // per_group), at_lane(me_e + fine_at)
    named = mask_buf[pl.ds(me_t * ET, ET)].reshape(CB, LANES)

    def share(inside, own_logit):
        terms = jnp.exp(jnp.where(inside, slot_logits - own_logit, -jnp.inf))
        return 1.0 / jnp.sum(terms, axis=1, keepdims=True)

    shares = share(lanes < GROUPS, own_group) * share(
        (named > 0.0) | (lanes == me_e + fine_at), own_fine
    )
    egate, eup = egate * slot_scale, eup * slot_scale
    ehid_buf[me_t] = (jax.nn.silu(egate) * eup * shares).astype(jnp.bfloat16)

    def hid_copy(n, k, owner, device):
        buf = (hid_buf, ehid_buf)[k]
        return remote(
            buf.at[owner], buf.at[owner], hid_s.at[n, k], hid_r.at[n, k], {"tp": device}
        )

    hid_copies = {}
    for n, (owner, device) in enumerate([(me_t, across), (me_t, partner), (across, partner)]):
        for k in range(2):
            hid_copies[n, k] = hid_copy(n, k, owner, device)
    for n in range(2):
        for k in range(2):
            hid_copies[n, k].start()
    for load in loads[4:6]:
        load.wait()

    def output_of(d):
        back = pick_buf[d].T[:S].astype(jnp.bfloat16)
        return dense_buf[d] + dot(back, eout_buf[d].astype(jnp.bfloat16))

    def finish(d):
        fin_send[d] = output_of(d).astype(jnp.bfloat16)
        fin_copy(d).start()

    def block_out(owner):
        blocks = pl.ds(owner * ET, ET)
        dense_buf[blocks] = dot(hid_buf[owner], dd[...]).reshape(ET, S, W)
        eout_buf[blocks] = dot(ehid_buf[owner], ed[...]).reshape(ET, slots, W)
        block_of(owner, from_others(finish))

    block_out(me_t)
    for k in range(2):
        hid_copies[1, k].wait_recv()
    block_out(partner)
    for k in range(2):
        hid_copies[0, k].wait_recv()
        hid_copies[2, k].start()
    block_out(across)
    for k in range(2):
        hid_copies[2, k].wait_recv()
    block_out(opposite)
    resid_buf[...] += output_of(0)

    def collect(d):
        fin_copy(d).wait_recv()
        resid_buf[...] += fin_recv[d].astype(jnp.float32)

    each(1, collect)
    out_ref[...] = resid_buf[...].astype(jnp.bfloat16)

    for copy in tp_copies + list(pre_copies.values()) + list(hid_copies.values()):
        copy.wait_send()
    each(1, lambda d: route_copy(d).wait_send())
    each(1, lambda d: row_copy(d).wait_send())
    each(1, lambda d: fin_copy(d).wait_send())


def tail(partial, tokens, first_gain, gain, w_key, w_value, routes, w_group, w_fine, w_mix, dg, du, dd, eg, eu, ed):
    E, T = lax.axis_size("ep"), lax.axis_size("tp")
    S, D = tokens.shape
    W, U = dg.shape
    F = eg.shape[1]
    per_group = E // GROUPS
    capacity = max(2, (S + per_group - 1) // per_group)
    slots = (capacity + 7) // 8 * 8
    ET = E // T
    RB, CB = ET * S, ET * slots
    KD = w_key.shape[1]
    bf16, f32 = jnp.bfloat16, jnp.float32
    vmem = pl.BlockSpec(memory_space=pltpu.VMEM)
    anywhere = pl.BlockSpec(memory_space=pltpu.HBM)
    dma = pltpu.SemaphoreType.DMA
    dims = (E, T, S, W, U, F, slots, per_group, w_fine.shape[1])
    return pl.pallas_call(
        functools.partial(tail_kernel, dims),
        out_shape=(
            jax.ShapeDtypeStruct((S, W), bf16),
            jax.ShapeDtypeStruct((S, KD), bf16),
            jax.ShapeDtypeStruct((S, KD), bf16),
        ),
        in_specs=[vmem] * 8 + [anywhere] * 8,
        out_specs=(vmem, vmem, vmem),
        scratch_shapes=[
            pltpu.VMEM((W, U), bf16), pltpu.VMEM((W, U), bf16), pltpu.VMEM((U, W), bf16),
            pltpu.VMEM((W, F), bf16), pltpu.VMEM((W, F), bf16), pltpu.VMEM((F, W), bf16),
            pltpu.VMEM((KD, D), bf16), pltpu.VMEM((KD, D), bf16), pltpu.VMEM((LANES, W), bf16),
            pltpu.VMEM((E, 8, LANES), f32),
            pltpu.VMEM((T - 1, S, W), bf16),
            pltpu.VMEM((S, W), f32),
            pltpu.VMEM((E, S, W), bf16),
            pltpu.VMEM((E, slots, LANES), f32),
            pltpu.VMEM((E, slots, LANES), f32),
            pltpu.VMEM((E, slots, W), f32),
            pltpu.VMEM((3, RB, U), bf16), pltpu.VMEM((3, RB, U), bf16),
            pltpu.VMEM((3, RB, U), bf16), pltpu.VMEM((3, RB, U), bf16),
            pltpu.VMEM((3, CB, 2 * F), bf16), pltpu.VMEM((3, CB, 2 * F), bf16),
            pltpu.VMEM((3, RB + CB, LANES), f32), pltpu.VMEM((3, RB + CB, LANES), f32),
            pltpu.VMEM((T, RB, U), bf16), pltpu.VMEM((T, CB, F), bf16),
            pltpu.VMEM((E, S, W), f32), pltpu.VMEM((E, slots, W), f32),
            pltpu.VMEM((E, S, W), bf16), pltpu.VMEM((E, S, W), bf16),
            dma((8,)), dma((E,)), dma((E,)), dma((T - 1,)), dma((T - 1,)), dma((E,)), dma((E,)),
            dma((3, 4)), dma((3, 4)), dma((3, 2)), dma((3, 2)),
            dma((E,)), dma((E,)),
        ],
        compiler_params=pltpu.CompilerParams(
            collective_id=0, has_side_effects=True, vmem_limit_bytes=48 * 1024 * 1024
        ),
        name="tail",
    )(
        partial, tokens, first_gain[None, :], gain[None, :], routes.T, w_group.T, w_fine.T,
        w_mix[None, :], dg, du, dd, eg, eu, ed, w_key.T, w_value.T,
    )


def shards(
    tokens,
    norm_attn,
    w_query,
    w_key,
    w_value,
    w_out,
    head_bias,
    key_cache,
    value_cache,
    lengths,
    norm_ffn,
    w_group,
    w_fine,
    routes,
    e_gate,
    e_up,
    e_down,
    d_gate,
    d_up,
    d_down,
    w_mix,
):
    seq_count = tokens.shape[0]
    kv_local = key_cache.shape[1]
    head_dim = key_cache.shape[3]
    h_first = normed(tokens, norm_attn).astype(jnp.bfloat16)
    queries = jnp.dot(h_first, w_query, preferred_element_type=jnp.float32).astype(jnp.bfloat16)
    heads_out = stick_read(
        queries.reshape(seq_count, -1, head_dim),
        jnp.swapaxes(key_cache[:, 0], 1, 2), jnp.swapaxes(value_cache[:, 0], 1, 2),
        lengths, head_bias,
    )
    partial_value = jnp.dot(heads_out, w_out, preferred_element_type=jnp.float32).astype(
        jnp.bfloat16
    )
    mixed, new_keys, new_values = tail(
        partial_value, tokens, norm_attn, norm_ffn, w_key, w_value, routes, w_group, w_fine, w_mix,
        d_gate, d_up, d_down, e_gate[0], e_up[0], e_down[0],
    )
    return (
        mixed,
        new_keys.reshape(seq_count, kv_local, head_dim),
        new_values.reshape(seq_count, kv_local, head_dim),
    )


def solution(mesh):
    placed = (
        P("ep", None),
        P(),
        P(None, "tp"),
        P(None, "tp"),
        P(None, "tp"),
        P("tp", None),
        P("tp"),
        P("ep", "tp", None, None),
        P("ep", "tp", None, None),
        P("ep"),
        P(),
        P(),
        P(),
        P("ep", None),
        P("ep", "tp", None),
        P("ep", "tp", None),
        P("ep", None, "tp"),
        P("tp", "ep"),
        P("tp", "ep"),
        P("ep", "tp"),
        P(),
    )
    return jax.shard_map(
        shards,
        mesh=mesh,
        in_specs=placed,
        out_specs=(P("ep", "tp"), P("ep", "tp", None), P("ep", "tp", None)),
        check_vma=False,
    )
```

```python
import jax
import jax.numpy as jnp
from jax import lax
from jax.experimental import pallas as pl
from jax.experimental.pallas import tpu as pltpu
from jax.sharding import PartitionSpec as P
import functools

GROUPS = 4
TOP_K = 2


norm_eps = 1e-06


def normed(values, gains):
    wide = values.astype(jnp.float32)
    return wide * lax.rsqrt(jnp.mean(wide * wide, axis=-1, keepdims=True) + norm_eps) * gains


def stick_kernel(batch, heads, lengths_ref, bias_ref, q_ref, k_ref, v_ref, out_ref):
    step = pl.program_id(0)
    head_dim, length = k_ref.shape[1:]
    pieces = length // LANES
    rows = batch * heads
    head = lax.broadcasted_iota(jnp.int32, (heads, length), 0)
    position = lax.broadcasted_iota(jnp.int32, (heads, length), 1)
    bias = jnp.zeros((heads, length), jnp.float32)
    for h in range(heads):
        bias = jnp.where(head == h, bias_ref[h], bias)
    parts, insides = [], []
    for i in range(batch):
        product = jnp.dot(q_ref[i], k_ref[i], preferred_element_type=jnp.float32)
        parts.append(product * head_dim ** (-0.5) + bias)
        insides.append((position < lengths_ref[step * batch + i]).astype(jnp.float32))
    scores = jnp.concatenate(parts, axis=0)
    inside = jnp.concatenate(insides, axis=0) > 0.0
    log_fail = -(jnp.maximum(scores, 0.0) + jnp.log1p(jnp.exp(-jnp.abs(scores))))
    fails = jnp.where(inside, log_fail, 0.0)
    stacked = jnp.concatenate(
        [fails[:, p * LANES : (p + 1) * LANES] for p in range(pieces)], axis=0
    )
    later = (
        lax.broadcasted_iota(jnp.int32, (LANES, LANES), 0)
        > lax.broadcasted_iota(jnp.int32, (LANES, LANES), 1)
    ).astype(jnp.float32).astype(jnp.bfloat16)
    within, left = jnp.zeros_like(stacked), stacked
    for _ in range(3):
        part = left.astype(jnp.bfloat16)
        left = left - part.astype(jnp.float32)
        within = within + jnp.dot(part, later, preferred_element_type=jnp.float32)
    totals = jnp.sum(stacked, axis=1, keepdims=True)
    carry, sums = jnp.zeros((rows, 1), jnp.float32), [None] * pieces
    for p in reversed(range(pieces)):
        sums[p] = within[p * rows : (p + 1) * rows] + carry
        carry = carry + totals[p * rows : (p + 1) * rows]
    suffix = jnp.concatenate(sums, axis=1)
    stick = jnp.where(inside, jnp.exp(scores + log_fail + suffix), 0.0)
    for i in range(batch):
        out_ref[i] = lax.dot_general(
            stick[i * heads : (i + 1) * heads].astype(jnp.bfloat16), v_ref[i],
            (((1,), (1,)), ((), ())), preferred_element_type=jnp.float32,
        ).astype(jnp.bfloat16)


def stick_read(queries, keys, values, lengths, bias):
    count, heads, head_dim = queries.shape
    length = keys.shape[2]
    batch = next(b for b in (4, 3, 2, 1) if count % b == 0)
    smem = pl.BlockSpec(memory_space=pltpu.SMEM)
    cache = pl.BlockSpec((batch, head_dim, length), lambda i: (i, 0, 0))
    small = pl.BlockSpec((batch, heads, head_dim), lambda i: (i, 0, 0))
    return pl.pallas_call(
        functools.partial(stick_kernel, batch, heads),
        grid=(count // batch,),
        out_shape=jax.ShapeDtypeStruct(queries.shape, jnp.bfloat16),
        in_specs=[smem, smem, small, cache, cache],
        out_specs=small,
        cost_estimate=pl.CostEstimate(
            flops=4 * count * heads * head_dim * length,
            bytes_accessed=4 * count * head_dim * length,
            transcendentals=3 * count * heads * length,
        ),
        name="stick",
    )(lengths, bias, queries, keys, values).reshape(count, -1)


LANES = 128
VMEM_BYTES = 67043328
MESH = pl.DeviceIdType.MESH


def tail_kernel(
    dims,
    partial_ref, tokens_ref, first_gain_ref, gain_ref, routes_ref, group_ref, fine_ref, mix_ref,
    dg_hbm, du_hbm, dd_hbm, eg_hbm, eu_hbm, ed_hbm, key_hbm, value_hbm,
    out_ref, key_out, value_out,
    dg, du, dd, eg, eu, ed, key_w, value_w, aux_w,
    route_buf, tp_buf, resid_buf, rows_buf, pick_buf, mask_buf, chosen_buf,
    gsend, grecv, usend, urecv, esend, erecv, asend, arecv,
    hid_buf, ehid_buf, dense_buf, eout_buf, fin_send, fin_recv,
    load_sem, rt_s, rt_r, tp_s, tp_r, row_s, row_r, pre_s, pre_r, hid_s, hid_r, fin_s, fin_r,
):
    E, T, S, W, U, F, slots, per_group, fine_count = dims
    ET = E // T
    RB, CB = ET * S, ET * slots
    me_e, me_t = lax.axis_index("ep"), lax.axis_index("tp")

    loads = [
        pltpu.make_async_copy(src, dst, load_sem.at[i])
        for i, (src, dst) in enumerate(
            [(dg_hbm, dg), (du_hbm, du), (eg_hbm, eg), (eu_hbm, eu), (dd_hbm, dd), (ed_hbm, ed),
             (key_hbm, key_w), (value_hbm, value_w)]
        )
    ]
    for load in loads[6:] + loads[:6]:
        load.start()

    barrier = pltpu.get_barrier_semaphore()

    def greet(d, carry):
        pl.semaphore_signal(
            barrier, inc=1, device_id={"ep": lax.rem(me_e + d, E)}, device_id_type=MESH
        )
        return carry

    lax.fori_loop(1, E, greet, 0)
    for j in range(1, T):
        pl.semaphore_signal(
            barrier, inc=1, device_id={"tp": lax.rem(me_t + j, T)}, device_id_type=MESH
        )
    feature_rows = pl.ds(pl.multiple_of(me_t * W, LANES), W)
    fine_at = 16
    mix = fine_at + (fine_count + 15) // 16 * 16
    mix_w = mix_ref[:, feature_rows]
    high = mix_w.astype(jnp.bfloat16)
    aux_w[...] = jnp.zeros_like(aux_w)
    aux_w[:GROUPS] = group_ref[:, feature_rows]
    aux_w[fine_at : fine_at + fine_count] = fine_ref[:, feature_rows]
    aux_w[mix : mix + 1] = high
    aux_w[mix + 16 : mix + 17] = (mix_w - high.astype(jnp.float32)).astype(jnp.bfloat16)
    route_buf[0] = jnp.full((8, LANES), -1.0, jnp.float32)
    route_buf[0, :TOP_K, :S] = routes_ref[...].astype(jnp.float32)
    pl.semaphore_wait(barrier, E - 1 + T - 1)

    def remote(src, dst, send, recv, device):
        return pltpu.make_async_remote_copy(
            src_ref=src, dst_ref=dst, send_sem=send, recv_sem=recv,
            device_id=device, device_id_type=MESH,
        )

    def feature_block(index):
        return pl.ds(pl.multiple_of(index * W, LANES), W)

    tp_copies = []
    for j in range(1, T):
        peer = lax.rem(me_t + j, T)
        tp_copies.append(
            remote(
                partial_ref.at[:, feature_block(peer)], tp_buf.at[j - 1],
                tp_s.at[j - 1], tp_r.at[j - 1], {"tp": peer},
            )
        )
        tp_copies[-1].start()

    def route_copy(d):
        return remote(
            route_buf.at[0], route_buf.at[d], rt_s.at[d], rt_r.at[d], {"ep": lax.rem(me_e + d, E)}
        )

    def row_copy(d):
        return remote(
            rows_buf.at[0], rows_buf.at[d], row_s.at[d], row_r.at[d], {"ep": lax.rem(me_e + d, E)}
        )

    def fin_copy(d):
        return remote(
            fin_send.at[d], fin_recv.at[d], fin_s.at[d], fin_r.at[d],
            {"ep": lax.rem(me_e - d + E, E)},
        )

    def each(first, body):
        def step(d, carry):
            body(d)
            return carry

        lax.fori_loop(first, E, step, 0)

    each(1, lambda d: route_copy(d).start())

    def dot(a, b):
        return jnp.dot(a, b, preferred_element_type=jnp.float32)

    def dot_t(a, b):
        return lax.dot_general(
            a, b, (((1,), (1,)), ((), ())), preferred_element_type=jnp.float32
        )

    for load in loads[6:]:
        load.wait()
    h_first = normed(tokens_ref[...], first_gain_ref[...]).astype(jnp.bfloat16)
    key_out[...] = dot_t(h_first, key_w[...]).astype(jnp.bfloat16)
    value_out[...] = dot_t(h_first, value_w[...]).astype(jnp.bfloat16)

    gain = gain_ref[:, feature_block(me_t)]
    total = tokens_ref[:, feature_block(me_t)].astype(jnp.float32)
    total = total + partial_ref[:, feature_block(me_t)].astype(jnp.float32)
    for j in range(1, T):
        tp_copies[j - 1].wait_recv()
        total = total + tp_buf[j - 1].astype(jnp.float32)
    resid_buf[...] = total
    rows_buf[0] = (total * gain).astype(jnp.bfloat16)

    partner = me_t + 1 - 2 * lax.rem(me_t, 2)
    across = lax.rem(me_t + T // 2, T)
    opposite = lax.rem(partner + T // 2, T)

    def block_of(owner, body):
        def step(i, carry):
            body(owner * ET + i)
            return carry

        lax.fori_loop(0, ET, step, 0)

    def from_others(body):
        def guarded(d):
            @pl.when(d > 0)
            def _():
                body(d)

        return guarded

    for owner in (opposite, across, partner, me_t):
        block_of(owner, from_others(lambda d: row_copy(d).start()))

    each(1, lambda d: route_copy(d).wait_recv())
    own = me_e.astype(jnp.float32)
    before = (
        lax.broadcasted_iota(jnp.int32, (LANES, LANES), 0)
        < lax.broadcasted_iota(jnp.int32, (LANES, LANES), 1)
    ).astype(jnp.float32).astype(jnp.bfloat16)
    slot_iota = lax.broadcasted_iota(jnp.int32, (slots, LANES), 0).astype(jnp.float32)
    lane_iota = lax.broadcasted_iota(jnp.int32, (slots, LANES), 1).astype(jnp.float32)

    def pick(d):
        named = route_buf[d]
        hits = jnp.where(named == own, 1.0, 0.0)
        ranks = jnp.dot(hits.astype(jnp.bfloat16), before, preferred_element_type=jnp.float32)
        rank = jnp.sum(ranks, axis=0, keepdims=True)
        hit = jnp.sum(hits, axis=0, keepdims=True)
        picks = jnp.where(slot_iota == rank, 1.0, 0.0) * hit
        pick_buf[d] = picks
        mask = jnp.zeros((slots, LANES), jnp.float32)
        for i in range(TOP_K):
            chosen = jnp.sum(picks * named[i : i + 1, :], axis=1, keepdims=True)
            mask = jnp.where(lane_iota == chosen + float(fine_at), 1.0, mask)
        mask_buf[d] = mask

    each(0, pick)

    def gather(d):
        chosen_buf[d] = jnp.dot(
            pick_buf[d][:, :S].astype(jnp.bfloat16), rows_buf[d],
            preferred_element_type=jnp.float32,
        )

    def gather_arrived(d):
        @pl.when(d > 0)
        def _():
            row_copy(d).wait_recv()

        gather(d)

    for load in loads[:4]:
        load.wait()

    inverse = 1.0 / gain

    def partials(owner):
        block_of(owner, gather_arrived)
        rows = rows_buf[pl.ds(owner * ET, ET)].astype(jnp.float32).reshape(RB, W)
        picked = chosen_buf[pl.ds(owner * ET, ET)].reshape(CB, W)
        both = jnp.concatenate([rows, picked], axis=0)
        scaled = both * inverse
        squares = jnp.sum(scaled * scaled, axis=1, keepdims=True)
        rows, picked = rows.astype(jnp.bfloat16), picked.astype(jnp.bfloat16)
        lanes = lax.broadcasted_iota(jnp.int32, (RB + CB, LANES), 1)
        aux = dot_t(both.astype(jnp.bfloat16), aux_w[...]) + jnp.where(lanes == LANES - 1, squares, 0.0)
        return rows, picked, aux

    pairs = [(gsend, grecv), (usend, urecv), (esend, erecv), (asend, arecv)]
    pre_copies = {}

    def send(n, k, value, device):
        src, dst = pairs[k]
        src[n] = value.astype(src.dtype)
        pre_copies[n, k] = remote(
            src.at[n], dst.at[n], pre_s.at[n, k], pre_r.at[n, k], {"tp": device}
        )
        pre_copies[n, k].start()

    def products(owner, consume):
        rows, picked, aux = partials(owner)
        consume(0, dot(rows, dg[...]))
        consume(1, dot(rows, du[...]))
        consume(2, jnp.concatenate([dot(picked, eg[...]), dot(picked, eu[...])], axis=1))
        consume(3, aux)

    def arrived(n, k):
        pre_copies[n, k].wait_recv()
        return pairs[k][1][n].astype(jnp.float32)

    products(opposite, lambda k, value: send(0, k, value, partner))
    products(across, lambda k, value: send(1, k, value + arrived(0, k), across))
    products(partner, lambda k, value: send(2, k, value, partner))
    kept = {}

    def keep(k, value):
        kept[k] = value + arrived(2, k)

    products(me_t, keep)
    gate, up, both_e, aux = [kept[k] + arrived(1, k) for k in range(4)]
    egate, eup = both_e[:, :F], both_e[:, F:]
    scale = lax.rsqrt(aux[:, LANES - 1 :] / (T * W) + norm_eps)
    logits = aux * scale
    mix_gate = jax.nn.sigmoid(logits[:RB, mix : mix + 1] + logits[:RB, mix + 16 : mix + 17])
    dense_scale, slot_scale = scale[:RB], scale[RB:]
    gate, up = gate * dense_scale, up * dense_scale
    hid_buf[me_t] = (jax.nn.silu(gate) * up * mix_gate).astype(jnp.bfloat16)

    slot_logits = logits[RB:]
    lanes = lax.broadcasted_iota(jnp.int32, (CB, LANES), 1)

    def at_lane(lane):
        return jnp.sum(jnp.where(lanes == lane, slot_logits, 0.0), axis=1, keepdims=True)

    own_group, own_fine = at_lane(me_e // per_group), at_lane(me_e + fine_at)
    named = mask_buf[pl.ds(me_t * ET, ET)].reshape(CB, LANES)

    def share(inside, own_logit):
        terms = jnp.exp(jnp.where(inside, slot_logits - own_logit, -jnp.inf))
        return 1.0 / jnp.sum(terms, axis=1, keepdims=True)

    shares = share(lanes < GROUPS, own_group) * share(
        (named > 0.0) | (lanes == me_e + fine_at), own_fine
    )
    egate, eup = egate * slot_scale, eup * slot_scale
    ehid_buf[me_t] = (jax.nn.silu(egate) * eup * shares).astype(jnp.bfloat16)

    def hid_copy(n, k, owner, device):
        buf = (hid_buf, ehid_buf)[k]
        return remote(
            buf.at[owner], buf.at[owner], hid_s.at[n, k], hid_r.at[n, k], {"tp": device}
        )

    hid_copies = {}
    for n, (owner, device) in enumerate([(me_t, across), (me_t, partner), (across, partner)]):
        for k in range(2):
            hid_copies[n, k] = hid_copy(n, k, owner, device)
    for n in range(2):
        for k in range(2):
            hid_copies[n, k].start()
    for load in loads[4:6]:
        load.wait()

    def output_of(d):
        back = pick_buf[d].T[:S].astype(jnp.bfloat16)
        return dense_buf[d] + dot(back, eout_buf[d].astype(jnp.bfloat16))

    def finish(d):
        fin_send[d] = output_of(d).astype(jnp.bfloat16)
        fin_copy(d).start()

    def block_out(owner):
        blocks = pl.ds(owner * ET, ET)
        dense_buf[blocks] = dot(hid_buf[owner], dd[...]).reshape(ET, S, W)
        eout_buf[blocks] = dot(ehid_buf[owner], ed[...]).reshape(ET, slots, W)
        block_of(owner, from_others(finish))

    block_out(me_t)
    for k in range(2):
        hid_copies[1, k].wait_recv()
    block_out(partner)
    for k in range(2):
        hid_copies[0, k].wait_recv()
        hid_copies[2, k].start()
    block_out(across)
    for k in range(2):
        hid_copies[2, k].wait_recv()
    block_out(opposite)
    resid_buf[...] += output_of(0)

    def collect(d):
        fin_copy(d).wait_recv()
        resid_buf[...] += fin_recv[d].astype(jnp.float32)

    each(1, collect)
    out_ref[...] = resid_buf[...].astype(jnp.bfloat16)

    for copy in tp_copies + list(pre_copies.values()) + list(hid_copies.values()):
        copy.wait_send()
    each(1, lambda d: route_copy(d).wait_send())
    each(1, lambda d: row_copy(d).wait_send())
    each(1, lambda d: fin_copy(d).wait_send())


def tail(partial, tokens, first_gain, gain, w_key, w_value, routes, w_group, w_fine, w_mix, dg, du, dd, eg, eu, ed):
    E, T = lax.axis_size("ep"), lax.axis_size("tp")
    S, D = tokens.shape
    W, U = dg.shape
    F = eg.shape[1]
    per_group = E // GROUPS
    capacity = max(2, (S + per_group - 1) // per_group)
    slots = (capacity + 7) // 8 * 8
    ET = E // T
    RB, CB = ET * S, ET * slots
    KD = w_key.shape[1]
    bf16, f32 = jnp.bfloat16, jnp.float32
    vmem = pl.BlockSpec(memory_space=pltpu.VMEM)
    anywhere = pl.BlockSpec(memory_space=pltpu.HBM)
    dma = pltpu.SemaphoreType.DMA
    dims = (E, T, S, W, U, F, slots, per_group, w_fine.shape[1])
    return pl.pallas_call(
        functools.partial(tail_kernel, dims),
        out_shape=(
            jax.ShapeDtypeStruct((S, W), bf16),
            jax.ShapeDtypeStruct((S, KD), bf16),
            jax.ShapeDtypeStruct((S, KD), bf16),
        ),
        in_specs=[vmem] * 8 + [anywhere] * 8,
        out_specs=(vmem, vmem, vmem),
        scratch_shapes=[
            pltpu.VMEM((W, U), bf16), pltpu.VMEM((W, U), bf16), pltpu.VMEM((U, W), bf16),
            pltpu.VMEM((W, F), bf16), pltpu.VMEM((W, F), bf16), pltpu.VMEM((F, W), bf16),
            pltpu.VMEM((KD, D), bf16), pltpu.VMEM((KD, D), bf16), pltpu.VMEM((LANES, W), bf16),
            pltpu.VMEM((E, 8, LANES), f32),
            pltpu.VMEM((T - 1, S, W), bf16),
            pltpu.VMEM((S, W), f32),
            pltpu.VMEM((E, S, W), bf16),
            pltpu.VMEM((E, slots, LANES), f32),
            pltpu.VMEM((E, slots, LANES), f32),
            pltpu.VMEM((E, slots, W), f32),
            pltpu.VMEM((3, RB, U), bf16), pltpu.VMEM((3, RB, U), bf16),
            pltpu.VMEM((3, RB, U), bf16), pltpu.VMEM((3, RB, U), bf16),
            pltpu.VMEM((3, CB, 2 * F), bf16), pltpu.VMEM((3, CB, 2 * F), bf16),
            pltpu.VMEM((3, RB + CB, LANES), f32), pltpu.VMEM((3, RB + CB, LANES), f32),
            pltpu.VMEM((T, RB, U), bf16), pltpu.VMEM((T, CB, F), bf16),
            pltpu.VMEM((E, S, W), f32), pltpu.VMEM((E, slots, W), f32),
            pltpu.VMEM((E, S, W), bf16), pltpu.VMEM((E, S, W), bf16),
            dma((8,)), dma((E,)), dma((E,)), dma((T - 1,)), dma((T - 1,)), dma((E,)), dma((E,)),
            dma((3, 4)), dma((3, 4)), dma((3, 2)), dma((3, 2)),
            dma((E,)), dma((E,)),
        ],
        compiler_params=pltpu.CompilerParams(
            collective_id=0, has_side_effects=True, vmem_limit_bytes=VMEM_BYTES
        ),
        name="tail",
    )(
        partial, tokens, first_gain[None, :], gain[None, :], routes.T, w_group.T, w_fine.T,
        w_mix[None, :], dg, du, dd, eg, eu, ed, w_key.T, w_value.T,
    )


def shards(
    tokens,
    norm_attn,
    w_query,
    w_key,
    w_value,
    w_out,
    head_bias,
    key_cache,
    value_cache,
    lengths,
    norm_ffn,
    w_group,
    w_fine,
    routes,
    e_gate,
    e_up,
    e_down,
    d_gate,
    d_up,
    d_down,
    w_mix,
):
    seq_count = tokens.shape[0]
    kv_local = key_cache.shape[1]
    head_dim = key_cache.shape[3]
    h_first = normed(tokens, norm_attn).astype(jnp.bfloat16)
    queries = jnp.dot(h_first, w_query, preferred_element_type=jnp.float32).astype(jnp.bfloat16)
    heads_out = stick_read(
        queries.reshape(seq_count, -1, head_dim),
        jnp.swapaxes(key_cache[:, 0], 1, 2), jnp.swapaxes(value_cache[:, 0], 1, 2),
        lengths, head_bias,
    )
    partial_value = jnp.dot(heads_out, w_out, preferred_element_type=jnp.float32).astype(
        jnp.bfloat16
    )
    mixed, new_keys, new_values = tail(
        partial_value, tokens, norm_attn, norm_ffn, w_key, w_value, routes, w_group, w_fine, w_mix,
        d_gate, d_up, d_down, e_gate[0], e_up[0], e_down[0],
    )
    return (
        mixed,
        new_keys.reshape(seq_count, kv_local, head_dim),
        new_values.reshape(seq_count, kv_local, head_dim),
    )


def solution(mesh):
    placed = (
        P("ep", None),
        P(),
        P(None, "tp"),
        P(None, "tp"),
        P(None, "tp"),
        P("tp", None),
        P("tp"),
        P("ep", "tp", None, None),
        P("ep", "tp", None, None),
        P("ep"),
        P(),
        P(),
        P(),
        P("ep", None),
        P("ep", "tp", None),
        P("ep", "tp", None),
        P("ep", None, "tp"),
        P("tp", "ep"),
        P("tp", "ep"),
        P("ep", "tp"),
        P(),
    )
    return jax.shard_map(
        shards,
        mesh=mesh,
        in_specs=placed,
        out_specs=(P("ep", "tp"), P("ep", "tp", None), P("ep", "tp", None)),
        check_vma=False,
    )
```
